32 devices in a mesh: tp: 8 (over z, y), dp: 4 (over x, core).
Axes of the slice: x: 2, y: 2, z: 4, core: 2. Of those that a mesh axis runs over, the one named last changes fastest.
Arguments:
- tokens: bfloat16 [128, 4096], P('dp', 'tp'), may hold values from -6 to 6
- lengths: int32 [128], P('dp'), may hold values from 1 to 96, 3072 in all
- norm_gain: float32 [2, 4096], replicated, may hold values from 0.1 to 1.9
- w_recept: bfloat16 [2, 4096, 4096], P(None, None, ('tp', 'dp')), may hold values from -0.09375 to 0.09375
- w_key: bfloat16 [2, 4096, 4096], P(None, None, ('tp', 'dp')), may hold values from -0.09375 to 0.09375
- w_value: bfloat16 [2, 4096, 4096], P(None, None, ('tp', 'dp')), may hold values from -0.09375 to 0.09375
- w_decay: bfloat16 [2, 4096, 4096], P(None, None, ('tp', 'dp')), may hold values from -0.09375 to 0.09375
- w_rate: bfloat16 [2, 4096, 4096], P(None, None, ('tp', 'dp')), may hold values from -0.09375 to 0.09375
- w_gate: bfloat16 [2, 4096, 4096], P(None, None, ('tp', 'dp')), may hold values from -0.09375 to 0.09375
- w_out: bfloat16 [2, 4096, 4096], P(None, None, ('tp', 'dp')), may hold values from -0.09375 to 0.09375
- decay_base: float32 [2, 4096], P(None, 'tp'), may hold values from -3 to 1
- rate_base: float32 [2, 4096], P(None, 'tp'), may hold values from -3 to 3
- group_gain: float32 [2, 4096], P(None, 'tp'), may hold values from 0.1 to 1.9
- state: float32 [2, 128, 64, 64, 64], P(None, 'dp', 'tp'), may hold values from -6 to 6
Outputs:
- mixed: bfloat16 [128, 4096], P('dp', 'tp')
- new_state: float32 [2, 128, 64, 64, 64], P(None, 'dp', 'tp')
The draws below stay inside these ranges and needn't reach their ends.
Inputs may be any that keep to these rules, and one draw needn't show every extreme that they name: Each sequence's live length lies between 1 and 96, some sequences reach 96, and the lengths sum to 3072.
All inputs are finite; a program needn't handle non-finite values.
Results may differ from the reference program's by a relative error of at most 0.025.
Values may be sent and summed in bfloat16 or wider, within the bound.
A program may use at most 128 MiB of HBM per device.

```python
import math
import jax
import jax.numpy as jnp
import numpy as np
from jax import lax

D = 4096
HEAD = 64
STEP = 16
BATCH = 128


def steps_of(key, extent, cuts, least, high):
    gain, own = 1.0, jax.random.fold_in(key, 6)
    for dim, blocks in cuts:
        heights = jnp.exp(jax.random.uniform(jax.random.fold_in(own, dim), (blocks,), jnp.float32, least / len(cuts), high / len(cuts)))
        gain = gain * jnp.repeat(heights, extent[dim] // blocks).reshape([-1 if axis == dim else 1 for axis in range(len(extent))])
    return gain


def profile(amount, total, reach, slope):
    loads = [(1 << 20) // math.isqrt(grade ** slope) + 1 for grade in range(2, amount + 1)]
    surplus, given = total - reach - (amount - 1), [1] * (amount - 1)
    while surplus > 0:
        candidates = [i for i in range(amount - 1) if given[i] < reach]
        pool, left = sum([loads[i] for i in candidates]), surplus
        for i in candidates:
            addition = min(reach - given[i], max(1, left * loads[i] // pool), surplus)
            given[i] = given[i] + addition
            surplus = surplus - addition
    return np.array([reach] + given)


def uneven_parts(key, amount, total, limit, slope):
    if amount == 2:
        one = jax.random.randint(key, (), max(1, total - limit), min(limit, total - 1) + 1)
        return jnp.stack([one, total - one])
    sizes = jnp.asarray(profile(amount, total, limit, slope), jnp.int32)
    couples = (amount - 1) // 2
    donor, receiver = sizes[1:1 + 2 * couples:2], sizes[2:2 + 2 * couples:2]
    room = jnp.minimum(donor - 1, limit - receiver)
    moved = jax.random.randint(jax.random.fold_in(key, 1), (couples,), 0, 1 << 20) % (room + 1)
    sizes = sizes.at[1:1 + 2 * couples:2].set(donor - moved).at[2:2 + 2 * couples:2].set(receiver + moved)
    return sizes[jax.random.permutation(jax.random.fold_in(key, 2), amount)]


def scatter_about(rng, dims, width, reach, pieces=(), dtype=jnp.bfloat16):
    level = steps_of(rng, dims, pieces, -0.22, 0.18) if pieces else 1.0
    values = jax.random.normal(rng, dims, jnp.float32) * width * level
    return jnp.minimum(jnp.maximum(values, -reach), reach).astype(dtype)


def setup_inputs(seed: int = 0) -> dict:
    splits = jax.random.split(jax.random.key(seed), 15)
    tokens = scatter_about(splits[0], (BATCH, D), 1.0, 6.0, ((0, 4), (1, 8)))
    lengths = uneven_parts(splits[1], BATCH, 24 * BATCH, 96, 2).astype(jnp.int32)
    norm_gain = jnp.clip(1.0 + 0.18 * jax.random.normal(splits[2], (2, D), jnp.float32), 0.1, 1.9)
    w_recept = scatter_about(splits[3], (2, D, D), D ** -0.5, 0.09375, ((2, 32),))
    w_key = scatter_about(splits[4], (2, D, D), D ** -0.5, 0.09375, ((2, 32),))
    w_value = scatter_about(splits[5], (2, D, D), D ** -0.5, 0.09375, ((2, 32),))
    w_decay = scatter_about(splits[6], (2, D, D), D ** -0.5, 0.09375, ((2, 32),))
    w_rate = scatter_about(splits[7], (2, D, D), D ** -0.5, 0.09375, ((2, 32),))
    w_gate = scatter_about(splits[8], (2, D, D), D ** -0.5, 0.09375, ((2, 32),))
    w_out = scatter_about(splits[9], (2, D, D), D ** -0.5, 0.09375, ((2, 32),))
    decay_base = jnp.clip(-3.0 + 4.0 * jax.random.uniform(splits[10], (2, D), jnp.float32) ** steps_of(splits[10], (2, D), ((1, 8),), -0.2, 0.2), -3.0, 1.0)
    rate_base = scatter_about(splits[11], (2, D), 0.5, 3.0, ((1, 8),), jnp.float32)
    group_gain = jnp.clip(1.0 + 0.18 * jax.random.normal(splits[12], (2, D), jnp.float32), 0.1, 1.9)
    state = scatter_about(splits[13], (2, BATCH, D // HEAD, HEAD, HEAD), 1.0, 6.0, ((1, 4), (2, 8)), jnp.float32)
    return dict(tokens=tokens, lengths=lengths, norm_gain=norm_gain, w_recept=w_recept, w_key=w_key, w_value=w_value, w_decay=w_decay, w_rate=w_rate, w_gate=w_gate, w_out=w_out, decay_base=decay_base, rate_base=rate_base, group_gain=group_gain, state=state)


RMS_EPS = 1e-06
GROUP_EPS = 0.00064

def stored(matrix, weight):
    product = jnp.dot(matrix, weight, preferred_element_type=jnp.float32)
    return lax.optimization_barrier(product.astype(jnp.bfloat16)).astype(jnp.float32)

def recur(state_old, recept, key_vec, value_vec, decay_rate, learn_rate, active, head_size):
    split = (recept.shape[0], -1, head_size)
    recept_h = recept.reshape(split)
    key_h = key_vec.reshape(split)
    value_h = value_vec.reshape(split)
    decay_h = decay_rate.reshape(split)
    rate_h = learn_rate.reshape(split)
    key_len = jnp.sqrt(lax.optimization_barrier(jnp.sum(key_h * key_h, axis=-1, keepdims=True)))
    key_unit = key_h / jnp.maximum(key_len, 1e-12)
    state_a = jnp.einsum('bhij,bhj->bhi', state_old, -key_unit, precision=lax.Precision.HIGHEST)
    updated = state_old * decay_h[:, :, None, :] + state_a[:, :, :, None] * (key_unit * rate_h)[:, :, None, :] + value_h[:, :, :, None] * (key_h * rate_h)[:, :, None, :]
    updated = jnp.where(active[:, None, None, None], updated, state_old)
    readout = jnp.einsum('bhij,bhj->bhi', updated, recept_h, precision=lax.Precision.HIGHEST)
    centre = lax.optimization_barrier(jnp.mean(readout, axis=-1, keepdims=True))
    spread = lax.optimization_barrier(jnp.mean(jnp.square(readout - centre), axis=-1, keepdims=True))
    normal_out = ((readout - centre) * lax.rsqrt(spread + GROUP_EPS)).reshape(recept.shape[0], -1)
    return (updated, normal_out)

def reference(tokens, lengths, norm_gain, w_recept, w_key, w_value, w_decay, w_rate, w_gate, w_out, decay_base, rate_base, group_gain, state):
    active = lengths > STEP
    current = tokens
    updated_states = []
    for layer_idx in range(2):
        values = current.astype(jnp.float32)
        factor = lax.rsqrt(lax.optimization_barrier(jnp.mean(values * values, axis=1, keepdims=True)) + RMS_EPS)
        normed = (values * factor * norm_gain[layer_idx]).astype(jnp.bfloat16)
        recept = stored(normed, w_recept[layer_idx])
        key_vec = stored(normed, w_key[layer_idx])
        value_vec = stored(normed, w_value[layer_idx])
        decay_pre = stored(normed, w_decay[layer_idx])
        rate_pre = stored(normed, w_rate[layer_idx])
        gate_pre = stored(normed, w_gate[layer_idx])
        decay_rate = jnp.exp(-jnp.exp(-jax.nn.softplus(-(decay_base[layer_idx] + decay_pre)) - 0.5))
        learn_rate = jax.nn.sigmoid(rate_base[layer_idx] + rate_pre)
        gate_open = jax.nn.sigmoid(gate_pre)
        updated, normal_out = recur(state[layer_idx], recept, key_vec, value_vec, decay_rate, learn_rate, active, HEAD)
        updated_states.append(updated)
        mixed_rows = jnp.where(active[:, None], normal_out * group_gain[layer_idx] * gate_open, 0.0).astype(jnp.bfloat16)
        current = jnp.dot(mixed_rows, w_out[layer_idx], preferred_element_type=jnp.float32).astype(jnp.bfloat16)
    return (current, jnp.stack(updated_states))
```

```python
import functools

import jax
import jax.numpy as jnp
from jax import lax
from jax.experimental import pallas as pl
from jax.experimental.pallas import tpu as pltpu
from jax.sharding import PartitionSpec as P

STEP = 16
RMS_EPS = 1e-06
GROUP_EPS = 0.00064
VMEM_LIMIT = 56 * 1024 * 1024


def project_body(x_ref, gain_ref, *refs, features, steps):
    weights, out_ref, acc, square = refs[:6], refs[6], refs[7], refs[8]
    step = pl.program_id(0)
    slim = weights[0].shape[-1]

    @pl.when(step == 0)
    def _():
        acc[...] = jnp.zeros_like(acc)
        square[...] = jnp.zeros_like(square)

    values = x_ref[...].astype(jnp.float32)
    square[...] += jnp.sum(values * values, axis=1, keepdims=True)
    scaled = (values * gain_ref[...]).astype(jnp.bfloat16)
    if slim % 128 == 0:
        joined = jnp.concatenate([w[0] for w in weights], axis=1)
        total = jnp.dot(scaled, joined, preferred_element_type=jnp.float32)
        for idx in range(6):
            acc[idx] += total[:, idx * slim : (idx + 1) * slim]
    else:
        for idx in range(6):
            acc[idx] += jnp.dot(scaled, weights[idx][0], preferred_element_type=jnp.float32)

    @pl.when(step == steps - 1)
    def _():
        factor = lax.rsqrt(square[...] / features + RMS_EPS)
        for idx in range(6):
            out_ref[idx] = (acc[idx] * factor).astype(out_ref.dtype)


def project(x, gain, weights, layer):
    rows, features = x.shape
    slim = weights[0].shape[2]
    depth = 512
    steps = features // depth
    return pl.pallas_call(
        functools.partial(project_body, features=features, steps=steps),
        grid=(steps,),
        out_shape=jax.ShapeDtypeStruct((6, rows, slim), jnp.bfloat16),
        in_specs=[
            pl.BlockSpec((rows, depth), lambda i: (0, i)),
            pl.BlockSpec((1, depth), lambda i: (0, i)),
        ]
        + [pl.BlockSpec((1, depth, slim), lambda i: (layer, i, 0))] * 6,
        out_specs=pl.BlockSpec((6, rows, slim), lambda i: (0, 0, 0)),
        scratch_shapes=[
            pltpu.VMEM((6, rows, slim), jnp.float32),
            pltpu.VMEM((rows, 1), jnp.float32),
        ],
        compiler_params=pltpu.CompilerParams(vmem_limit_bytes=VMEM_LIMIT),
        name="project",
    )(x, gain, *weights)


def fold_body(x_ref, w_ref, out_ref, acc, *, steps):
    step = pl.program_id(0)

    @pl.when(step == 0)
    def _():
        acc[...] = jnp.zeros_like(acc)

    acc[...] += jnp.dot(x_ref[...], w_ref[0], preferred_element_type=jnp.float32)

    @pl.when(step == steps - 1)
    def _():
        out_ref[...] = acc[...].astype(out_ref.dtype)


def fold(x, weight, layer):
    rows, features = x.shape
    slim = weight.shape[2]
    depth = 1024
    steps = features // depth
    return pl.pallas_call(
        functools.partial(fold_body, steps=steps),
        grid=(steps,),
        out_shape=jax.ShapeDtypeStruct((rows, slim), jnp.bfloat16),
        in_specs=[
            pl.BlockSpec((rows, depth), lambda i: (0, i)),
            pl.BlockSpec((1, depth, slim), lambda i: (layer, i, 0)),
        ],
        out_specs=pl.BlockSpec((rows, slim), lambda i: (0, 0)),
        scratch_shapes=[pltpu.VMEM((rows, slim), jnp.float32)],
        compiler_params=pltpu.CompilerParams(vmem_limit_bytes=VMEM_LIMIT),
        name="fold",
    )(x, weight)


def recur_body(vec_ref, lens_ref, base_ref, rate_ref, gain_ref, state_ref, *refs):
    new_ref, mixed_ref, rows_s, read_s = refs[-4:]
    group, heads, size = state_ref.shape[1], state_ref.shape[2], state_ref.shape[3]
    live = lens_ref[...] > STEP
    for h in range(heads):
        part = slice(h * size, (h + 1) * size)
        recept, key, value, decay_pre, rate_pre = [
            vec_ref[q, :, part].astype(jnp.float32) for q in range(5)
        ]
        decay = jnp.exp(-jnp.exp(-jax.nn.softplus(-(base_ref[:, part] + decay_pre)) - 0.5))
        rate = jax.nn.sigmoid(rate_ref[:, part] + rate_pre)
        length = jnp.maximum(jnp.sqrt(jnp.sum(key * key, axis=1, keepdims=True)), 1e-12)
        unit = key / length
        rows_s[0, h] = -unit
        rows_s[1, h] = value * length
        rows_s[2, h] = decay
        rows_s[3, h] = unit * rate
        rows_s[4, h] = recept
    across = lax.broadcasted_iota(jnp.int32, (size, size), 0)
    along = lax.broadcasted_iota(jnp.int32, (size, size), 1)
    eye = across == along

    def one(b, carry):
        keep = lens_ref[pl.ds(b, 1), :size] > STEP
        for h in range(heads):
            neg, held, decay, rated, recept = [rows_s[q, h, pl.ds(b, 1), :] for q in range(5)]
            old = state_ref[0, b, h]
            terms = old * neg + jnp.where(eye, held, 0.0)
            weight = jnp.sum(terms, axis=1, keepdims=True)
            updated = old * decay + weight * rated
            new_ref[0, b, h] = jnp.where(keep, updated, old)
            read = jnp.sum(updated * recept, axis=1, keepdims=True)
            read_s[h, pl.ds(b, 1), :] = jnp.sum(jnp.where(eye, read, 0.0), axis=0, keepdims=True)
        return carry

    lax.fori_loop(0, group, one, 0)
    for h in range(heads):
        part = slice(h * size, (h + 1) * size)
        read = read_s[h]
        centre = jnp.mean(read, axis=1, keepdims=True)
        apart = read - centre
        spread = jnp.mean(apart * apart, axis=1, keepdims=True)
        normal = apart * lax.rsqrt(spread + GROUP_EPS) * gain_ref[:, part]
        gate = jax.nn.sigmoid(vec_ref[5, :, part].astype(jnp.float32))
        mixed_ref[:, part] = jnp.where(live[:, :size], normal * gate, 0.0).astype(mixed_ref.dtype)


def recur(vec, lens, base, rate, gain, state, earlier, layer):
    _, rows, width = vec.shape
    heads, size = state.shape[2], state.shape[3]
    group = 8
    block = pl.BlockSpec((1, group, heads, size, size), lambda i: (layer, i, 0, 0, 0))
    line = pl.BlockSpec((1, width), lambda i: (0, 0))
    operands = [vec, lens, base, rate, gain, state]
    in_specs = [
        pl.BlockSpec((6, group, width), lambda i: (0, i, 0)),
        pl.BlockSpec((group, lens.shape[1]), lambda i: (i, 0)),
        line,
        line,
        line,
        block,
    ]
    aliases = {}
    if earlier is not None:
        operands.append(earlier)
        in_specs.append(pl.BlockSpec(memory_space=pl.ANY))
        aliases = {6: 0}
    return pl.pallas_call(
        recur_body,
        grid=(rows // group,),
        out_shape=(
            jax.ShapeDtypeStruct(state.shape, state.dtype),
            jax.ShapeDtypeStruct((rows, width), jnp.bfloat16),
        ),
        in_specs=in_specs,
        out_specs=(block, pl.BlockSpec((group, width), lambda i: (i, 0))),
        scratch_shapes=[
            pltpu.VMEM((5, heads, group, size), jnp.float32),
            pltpu.VMEM((heads, group, size), jnp.float32),
        ],
        input_output_aliases=aliases,
        compiler_params=pltpu.CompilerParams(vmem_limit_bytes=VMEM_LIMIT),
        name="recur",
    )(*operands)


def on_device(
    tokens,
    lengths,
    norm_gain,
    w_recept,
    w_key,
    w_value,
    w_decay,
    w_rate,
    w_gate,
    w_out,
    decay_base,
    rate_base,
    group_gain,
    state,
):
    weights = (w_recept, w_key, w_value, w_decay, w_rate, w_gate)
    lens = jnp.broadcast_to(lengths[:, None], (lengths.shape[0], 128))
    every = lax.all_gather(tokens, "dp", axis=0, tiled=True)
    every = lax.all_gather(every, "tp", axis=1, tiled=True)
    states = None
    for layer in range(2):
        pick = slice(layer, layer + 1)
        pieces = project(every, norm_gain[pick], weights, layer)
        vec = lax.all_to_all(pieces, "dp", split_axis=1, concat_axis=2, tiled=True)
        states, mixed = recur(
            vec, lens, decay_base[pick], rate_base[pick], group_gain[pick], state, states, layer
        )
        rows_all = lax.all_gather(mixed, "dp", axis=0, tiled=True)
        rows_all = lax.all_gather(rows_all, "tp", axis=1, tiled=True)
        columns = fold(rows_all, w_out, layer)
        if layer == 0:
            every = lax.all_gather(columns, ("tp", "dp"), axis=1, tiled=True)
    current = lax.all_to_all(columns, "dp", split_axis=0, concat_axis=1, tiled=True)
    return (current, states)


def solution(mesh):
    in_specs = (
        P("dp", "tp"),
        P("dp"),
        P(),
        P(None, None, ("tp", "dp")),
        P(None, None, ("tp", "dp")),
        P(None, None, ("tp", "dp")),
        P(None, None, ("tp", "dp")),
        P(None, None, ("tp", "dp")),
        P(None, None, ("tp", "dp")),
        P(None, None, ("tp", "dp")),
        P(None, "tp"),
        P(None, "tp"),
        P(None, "tp"),
        P(None, "dp", "tp", None, None),
    )
    out_specs = (P("dp", "tp"), P(None, "dp", "tp", None, None))
    return jax.shard_map(
        on_device, mesh=mesh, in_specs=in_specs, out_specs=out_specs, check_vma=False
    )
```

```python
import functools

import jax
import jax.numpy as jnp
from jax import lax
from jax.experimental import pallas as pl
from jax.experimental.pallas import tpu as pltpu
from jax.sharding import PartitionSpec as P

STEP = 16
RMS_EPS = 1e-06
GROUP_EPS = 0.00064
VMEM_LIMIT = 56 * 1024 * 1024


MESH = pl.DeviceIdType.MESH


def greet(peers):
    barrier = pltpu.get_barrier_semaphore()
    for tp, dp in peers:
        pl.semaphore_signal(barrier, inc=1, device_id=(tp, dp), device_id_type=MESH)
    pl.semaphore_wait(barrier, len(peers))


def gather_body(x_ref, out_ref, own_sem, send_sem, recv_sem, *, tp, dp):
    t, d = lax.axis_index("tp"), lax.axis_index("dp")
    core = lax.rem(d, 2)
    sibling = d + 1 - 2 * core
    others = [lax.rem(d + 2 * k, dp) for k in range(1, dp // 2)]
    sent = []

    def send(source, slot, to_t, to_d):
        copy = pltpu.make_async_remote_copy(
            src_ref=source,
            dst_ref=out_ref.at[slot],
            send_sem=send_sem.at[len(sent)],
            recv_sem=recv_sem.at[slot],
            device_id=(to_t, to_d),
            device_id_type=MESH,
        )
        copy.start()
        sent.append(copy)

    def arrived(slot):
        pltpu.make_async_remote_copy(
            src_ref=x_ref,
            dst_ref=out_ref.at[slot],
            send_sem=send_sem.at[0],
            recv_sem=recv_sem.at[slot],
            device_id=(t, sibling),
            device_id_type=MESH,
        ).wait_recv()

    rows = [lax.rem(t + k, tp) for k in range(1, tp)]
    greet([(r, d) for r in rows] + [(t, o) for o in others] + [(t, sibling)])
    mine = t * dp + d
    own = pltpu.make_async_copy(x_ref, out_ref.at[mine], own_sem)
    own.start()
    for r in rows:
        send(x_ref, mine, r, d)
    for o in others + [sibling]:
        send(x_ref, mine, t, o)
    for k in range(1, tp):
        slot = lax.rem(t + tp - k, tp) * dp + d
        arrived(slot)
        for o in others + [sibling]:
            send(out_ref.at[slot], slot, t, o)
    for k in range(tp):
        for o in others:
            slot = lax.rem(t + tp - k, tp) * dp + o
            arrived(slot)
            send(out_ref.at[slot], slot, t, sibling)
    for k in range(tp):
        for o in [d] + others:
            arrived(lax.rem(t + tp - k, tp) * dp + o + sibling - d)
    own.wait()
    for copy in sent:
        copy.wait_send()


def gather(x, tp, dp, number):
    count = (tp - 1) + tp * (dp // 2) + tp * (dp // 2 - 1)
    return pl.pallas_call(
        functools.partial(gather_body, tp=tp, dp=dp),
        out_shape=jax.ShapeDtypeStruct((tp * dp,) + x.shape, x.dtype),
        in_specs=[pl.BlockSpec(memory_space=pltpu.VMEM)],
        out_specs=pl.BlockSpec(memory_space=pltpu.VMEM),
        scratch_shapes=[
            pltpu.SemaphoreType.DMA,
            pltpu.SemaphoreType.DMA((count,)),
            pltpu.SemaphoreType.DMA((tp * dp,)),
        ],
        compiler_params=pltpu.CompilerParams(collective_id=number, has_side_effects=True),
        name="gather",
    )(x)


def exchange_body(x_ref, out_ref, own_sem, send_sem, recv_sem, *, dp):
    t, d = lax.axis_index("tp"), lax.axis_index("dp")
    peers = [lax.rem(d + k, dp) for k in range(1, dp)]
    greet([(t, o) for o in peers])
    own = pltpu.make_async_copy(x_ref.at[d], out_ref.at[d], own_sem)
    own.start()
    sent = []
    for k, o in enumerate(peers):
        copy = pltpu.make_async_remote_copy(
            src_ref=x_ref.at[o],
            dst_ref=out_ref.at[d],
            send_sem=send_sem.at[k],
            recv_sem=recv_sem.at[k],
            device_id=(t, o),
            device_id_type=MESH,
        )
        copy.start()
        sent.append(copy)
    for k in range(1, dp):
        source = lax.rem(d + dp - k, dp)
        pltpu.make_async_remote_copy(
            src_ref=x_ref.at[source],
            dst_ref=out_ref.at[source],
            send_sem=send_sem.at[k - 1],
            recv_sem=recv_sem.at[k - 1],
            device_id=(t, source),
            device_id_type=MESH,
        ).wait_recv()
    own.wait()
    for copy in sent:
        copy.wait_send()


def exchange(x, dp, number):
    return pl.pallas_call(
        functools.partial(exchange_body, dp=dp),
        out_shape=jax.ShapeDtypeStruct(x.shape, x.dtype),
        in_specs=[pl.BlockSpec(memory_space=pltpu.VMEM)],
        out_specs=pl.BlockSpec(memory_space=pltpu.VMEM),
        scratch_shapes=[
            pltpu.SemaphoreType.DMA,
            pltpu.SemaphoreType.DMA((dp - 1,)),
            pltpu.SemaphoreType.DMA((dp - 1,)),
        ],
        compiler_params=pltpu.CompilerParams(collective_id=number, has_side_effects=True),
        name="exchange",
    )(x)


def joined_block(x_ref, across):
    if across:
        return jnp.concatenate([x_ref[j] for j in range(x_ref.shape[0])], axis=1)
    return x_ref[...].reshape(x_ref.shape[0] * x_ref.shape[1], x_ref.shape[2])


def project_body(x_ref, gain_ref, *refs, features, steps, across):
    weights, out_ref, acc, square = refs[:6], refs[6], refs[7], refs[8]
    step = pl.program_id(0)
    slim = weights[0].shape[-1]

    @pl.when(step == 0)
    def _():
        acc[...] = jnp.zeros_like(acc)
        square[...] = jnp.zeros_like(square)

    values = joined_block(x_ref, across).astype(jnp.float32)
    square[...] += jnp.sum(values * values, axis=1, keepdims=True)
    scaled = (values * gain_ref[...]).astype(jnp.bfloat16)
    if slim % 128 == 0:
        joined = jnp.concatenate([w[0] for w in weights], axis=1)
        total = jnp.dot(scaled, joined, preferred_element_type=jnp.float32)
        for idx in range(6):
            acc[idx] += total[:, idx * slim : (idx + 1) * slim]
    else:
        for idx in range(6):
            acc[idx] += jnp.dot(scaled, weights[idx][0], preferred_element_type=jnp.float32)

    @pl.when(step == steps - 1)
    def _():
        factor = lax.rsqrt(square[...] / features + RMS_EPS)
        for idx in range(6):
            done = (acc[idx] * factor).astype(out_ref.dtype)
            share = out_ref.shape[2]
            for j in range(out_ref.shape[0]):
                out_ref[j, idx] = done[j * share : (j + 1) * share]


def project(x, gain, weights, layer, steps, dp, across):
    features, slim = weights[0].shape[1:]
    part = x.shape[0] // steps
    depth = features // steps
    rows = x.shape[1] * (1 if across else part)
    return pl.pallas_call(
        functools.partial(project_body, features=features, steps=steps, across=across),
        grid=(steps,),
        out_shape=jax.ShapeDtypeStruct((dp, 6, rows // dp, slim), jnp.bfloat16),
        in_specs=[
            pl.BlockSpec((part,) + x.shape[1:], lambda i: (i, 0, 0)),
            pl.BlockSpec((1, depth), lambda i: (0, i)),
        ]
        + [pl.BlockSpec((1, depth, slim), lambda i: (layer, i, 0))] * 6,
        out_specs=pl.BlockSpec((dp, 6, rows // dp, slim), lambda i: (0, 0, 0, 0)),
        scratch_shapes=[
            pltpu.VMEM((6, rows, slim), jnp.float32),
            pltpu.VMEM((rows, 1), jnp.float32),
        ],
        compiler_params=pltpu.CompilerParams(vmem_limit_bytes=VMEM_LIMIT),
        name="project",
    )(x, gain, *weights)


def fold_body(x_ref, w_ref, out_ref, acc, *, steps):
    step = pl.program_id(0)

    @pl.when(step == 0)
    def _():
        acc[...] = jnp.zeros_like(acc)

    acc[...] += jnp.dot(joined_block(x_ref, False), w_ref[0], preferred_element_type=jnp.float32)

    @pl.when(step == steps - 1)
    def _():
        out_ref[...] = acc[...].astype(out_ref.dtype)


def fold(x, weight, layer, steps):
    features, slim = weight.shape[1:]
    part = x.shape[0] // steps
    depth = features // steps
    rows = part * x.shape[1]
    return pl.pallas_call(
        functools.partial(fold_body, steps=steps),
        grid=(steps,),
        out_shape=jax.ShapeDtypeStruct((rows, slim), jnp.bfloat16),
        in_specs=[
            pl.BlockSpec((part,) + x.shape[1:], lambda i: (i, 0, 0)),
            pl.BlockSpec((1, depth, slim), lambda i: (layer, i, 0)),
        ],
        out_specs=pl.BlockSpec((rows, slim), lambda i: (0, 0)),
        scratch_shapes=[pltpu.VMEM((rows, slim), jnp.float32)],
        compiler_params=pltpu.CompilerParams(vmem_limit_bytes=VMEM_LIMIT),
        name="fold",
    )(x, weight)


def recur_body(vec_ref, lens_ref, base_ref, rate_ref, gain_ref, state_ref, *refs):
    new_ref, mixed_ref, rows_s, read_s = refs[-4:]
    group, heads, size = state_ref.shape[1], state_ref.shape[2], state_ref.shape[3]
    live = lens_ref[...] > STEP
    for h in range(heads):
        part = slice(h * size, (h + 1) * size)
        recept, key, value, decay_pre, rate_pre = [
            vec_ref[q, :, part].astype(jnp.float32) for q in range(5)
        ]
        decay = jnp.exp(-jnp.exp(-jax.nn.softplus(-(base_ref[:, part] + decay_pre)) - 0.5))
        rate = jax.nn.sigmoid(rate_ref[:, part] + rate_pre)
        length = jnp.maximum(jnp.sqrt(jnp.sum(key * key, axis=1, keepdims=True)), 1e-12)
        unit = key / length
        rows_s[0, h] = -unit
        rows_s[1, h] = value * length
        rows_s[2, h] = decay
        rows_s[3, h] = unit * rate
        rows_s[4, h] = recept
    across = lax.broadcasted_iota(jnp.int32, (size, size), 0)
    along = lax.broadcasted_iota(jnp.int32, (size, size), 1)
    eye = across == along

    def one(b, carry):
        keep = lens_ref[pl.ds(b, 1), :size] > STEP
        for h in range(heads):
            neg, held, decay, rated, recept = [rows_s[q, h, pl.ds(b, 1), :] for q in range(5)]
            old = state_ref[0, b, h]
            terms = old * neg + jnp.where(eye, held, 0.0)
            weight = jnp.sum(terms, axis=1, keepdims=True)
            updated = old * decay + weight * rated
            new_ref[0, b, h] = jnp.where(keep, updated, old)
            read = jnp.sum(updated * recept, axis=1, keepdims=True)
            read_s[h, pl.ds(b, 1), :] = jnp.sum(jnp.where(eye, read, 0.0), axis=0, keepdims=True)
        return carry

    lax.fori_loop(0, group, one, 0)
    for h in range(heads):
        part = slice(h * size, (h + 1) * size)
        read = read_s[h]
        centre = jnp.mean(read, axis=1, keepdims=True)
        apart = read - centre
        spread = jnp.mean(apart * apart, axis=1, keepdims=True)
        normal = apart * lax.rsqrt(spread + GROUP_EPS) * gain_ref[:, part]
        gate = jax.nn.sigmoid(vec_ref[5, :, part].astype(jnp.float32))
        mixed_ref[:, part] = jnp.where(live[:, :size], normal * gate, 0.0).astype(mixed_ref.dtype)


def recur(vec, lens, base, rate, gain, state, earlier, layer):
    _, rows, width = vec.shape
    heads, size = state.shape[2], state.shape[3]
    group = 8
    block = pl.BlockSpec((1, group, heads, size, size), lambda i: (layer, i, 0, 0, 0))
    line = pl.BlockSpec((1, width), lambda i: (0, 0))
    operands = [vec, lens, base, rate, gain, state]
    in_specs = [
        pl.BlockSpec((6, group, width), lambda i: (0, i, 0)),
        pl.BlockSpec((group, lens.shape[1]), lambda i: (i, 0)),
        line,
        line,
        line,
        block,
    ]
    aliases = {}
    if earlier is not None:
        operands.append(earlier)
        in_specs.append(pl.BlockSpec(memory_space=pl.ANY))
        aliases = {6: 0}
    return pl.pallas_call(
        recur_body,
        grid=(rows // group,),
        out_shape=(
            jax.ShapeDtypeStruct(state.shape, state.dtype),
            jax.ShapeDtypeStruct((rows, width), jnp.bfloat16),
        ),
        in_specs=in_specs,
        out_specs=(block, pl.BlockSpec((group, width), lambda i: (i, 0))),
        scratch_shapes=[
            pltpu.VMEM((5, heads, group, size), jnp.float32),
            pltpu.VMEM((heads, group, size), jnp.float32),
        ],
        input_output_aliases=aliases,
        compiler_params=pltpu.CompilerParams(vmem_limit_bytes=VMEM_LIMIT),
        name="recur",
    )(*operands)


def on_device(
    tokens,
    lengths,
    norm_gain,
    w_recept,
    w_key,
    w_value,
    w_decay,
    w_rate,
    w_gate,
    w_out,
    decay_base,
    rate_base,
    group_gain,
    state,
):
    weights = (w_recept, w_key, w_value, w_decay, w_rate, w_gate)
    tp, dp = lax.axis_size("tp"), lax.axis_size("dp")
    rows, slim = lengths.shape[0], w_out.shape[2]
    lens = jnp.broadcast_to(lengths[:, None], (rows, 128))
    every, across = gather(tokens, tp, dp, 0), False
    states = None
    for layer in range(2):
        pick = slice(layer, layer + 1)
        pieces = project(every, norm_gain[pick], weights, layer, tp, dp, across)
        vec = exchange(pieces, dp, 1 + layer)
        vec = vec.transpose(1, 2, 0, 3).reshape(6, rows, dp * slim)
        states, mixed = recur(
            vec, lens, decay_base[pick], rate_base[pick], group_gain[pick], state, states, layer
        )
        columns = fold(gather(mixed, tp, dp, 3 + layer), w_out, layer, tp)
        if layer == 0:
            across = slim % 128 == 0
            if across:
                every = gather(columns, tp, dp, 5)
            else:
                every = lax.all_gather(columns, ("tp", "dp"), axis=1, tiled=True)
                every = every.reshape(dp * rows, tp, dp * slim).transpose(1, 0, 2)
    current = exchange(columns.reshape(dp, rows, slim), dp, 6)
    return (current.transpose(1, 0, 2).reshape(rows, dp * slim), states)


def solution(mesh):
    in_specs = (
        P("dp", "tp"),
        P("dp"),
        P(),
        P(None, None, ("tp", "dp")),
        P(None, None, ("tp", "dp")),
        P(None, None, ("tp", "dp")),
        P(None, None, ("tp", "dp")),
        P(None, None, ("tp", "dp")),
        P(None, None, ("tp", "dp")),
        P(None, None, ("tp", "dp")),
        P(None, "tp"),
        P(None, "tp"),
        P(None, "tp"),
        P(None, "dp", "tp", None, None),
    )
    out_specs = (P("dp", "tp"), P(None, "dp", "tp", None, None))
    return jax.shard_map(
        on_device, mesh=mesh, in_specs=in_specs, out_specs=out_specs, check_vma=False
    )
```
